32 devices in a mesh: tp: 4 (over z), dp: 8 (over y, x, core).
Axes of the slice: x: 2, y: 2, z: 4, core: 2. Of those that a mesh axis runs over, the one named last changes fastest.
Arguments:
- tokens: bfloat16 [64, 4096], P(None, 'dp'), may hold values from -6 to 6
- norm_gain: float32 [2, 4096], P(None, 'dp'), may hold values from 0.1 to 1.9
- w_gate: bfloat16 [2, 4096, 3072], P(None, 'dp', 'tp'), may hold values from -0.09375 to 0.09375
- w_value: bfloat16 [2, 4096, 3072], P(None, 'dp', 'tp'), may hold values from -0.09375 to 0.09375
- w_inmap: bfloat16 [2, 4096, 3072], P(None, 'dp', 'tp'), may hold values from -0.09375 to 0.09375
- w_readout: bfloat16 [2, 4096, 3072], P(None, 'dp', 'tp'), may hold values from -0.09375 to 0.09375
- w_step: bfloat16 [2, 4096, 48], P(None, 'dp'), may hold values from -0.09375 to 0.09375
- step_bias: float32 [2, 48], P(None, 'tp'), may hold values from -4 to 1
- decay_log: float32 [2, 48], P(None, 'tp'), may hold values from -1 to 2.5
- skip_gain: float32 [2, 48], P(None, 'tp'), may hold values from 0.5 to 2
- conv_taps: bfloat16 [2, 5, 3, 3072], P(None, None, None, 'tp'), may hold values from -2.5 to 2.5
- gate_gain: float32 [2, 3072], P(None, 'tp'), may hold values from 0.1 to 1.9
- w_project: bfloat16 [2, 3072, 4096], P(None, 'tp', 'dp'), may hold values from -0.109375 to 0.109375
- states: float32 [2, 64, 48, 4096], P(None, 'dp', 'tp'), may hold values from -3 to 3
- recent: bfloat16 [2, 64, 4, 3, 3072], P(None, 'dp', None, None, 'tp'), may hold values from -6 to 6
Outputs:
- next_tokens: bfloat16 [64, 4096], P(None, 'dp')
- next_states: float32 [2, 64, 48, 4096], P(None, 'dp', 'tp')
- next_recent: bfloat16 [2, 64, 4, 3, 3072], P(None, 'dp', None, None, 'tp')
The draws below stay inside these ranges and needn't reach their ends.
All inputs are finite; a program needn't handle non-finite values.
Results may differ from the reference program's by a relative error of at most 0.014.
Values may be sent and summed in bfloat16 or wider, within the bound.
A program may use at most 64 MiB of HBM per device.

```python
import jax
import jax.numpy as jnp
from jax import lax

D = 4096
HEADS = 48
HEAD_DIM = 64
STATE = 64
SSD_DIM = 3072
CONV = 5
LAYERS = 2
BATCH = 64


def shard_levels(stream_key, extent, split, low, high):
    loudness = 1.0
    for position, shards_of in split:
        heights = jax.random.uniform(jax.random.fold_in(jax.random.fold_in(stream_key, 6), position), (shards_of,), jnp.float32, low / len(split), high / len(split))
        loudness = loudness * jnp.repeat(jnp.exp(heights), extent[position] // shards_of).reshape((-1,) + (1,) * (len(extent) - 1 - position))
    return loudness


def scatter_about(own_key, extent, deviation, bound, split=(), dtype=jnp.bfloat16):
    values = jax.random.normal(own_key, extent, jnp.float32) * deviation
    if len(split) > 0:
        values = shard_levels(own_key, extent, split, -0.22, 0.18) * values
    return jnp.clip(values, min=-bound, max=bound).astype(dtype)


def setup_inputs(seed: int = 0) -> dict:
    key_of = jax.random.split(jax.random.key(seed), 16)
    return {
        "tokens": scatter_about(key_of[0], (BATCH, D), 1.0, 6.0, ((1, 8),)),
        "norm_gain": jnp.clip(1.0 + 0.18 * jax.random.normal(key_of[1], (LAYERS, D), jnp.float32), 0.1, 1.9),
        "w_gate": scatter_about(key_of[2], (LAYERS, D, SSD_DIM), D ** -0.5, 0.09375, ((1, 8), (2, 4))),
        "w_value": scatter_about(key_of[3], (LAYERS, D, SSD_DIM), D ** -0.5, 0.09375, ((1, 8), (2, 4))),
        "w_inmap": scatter_about(key_of[4], (LAYERS, D, SSD_DIM), D ** -0.5, 0.09375, ((1, 8), (2, 4))),
        "w_readout": scatter_about(key_of[5], (LAYERS, D, SSD_DIM), D ** -0.5, 0.09375, ((1, 8), (2, 4))),
        "w_step": scatter_about(key_of[6], (LAYERS, D, HEADS), D ** -0.5, 0.09375, ((1, 8),)),
        "step_bias": jnp.clip(-4.0 + 5.0 * jax.random.uniform(key_of[7], (LAYERS, HEADS), jnp.float32) ** shard_levels(key_of[7], (LAYERS, HEADS), ((1, 4),), -0.2, 0.2), -4.0, 1.0),
        "decay_log": jnp.clip(-1.0 + 3.5 * jax.random.uniform(key_of[8], (LAYERS, HEADS), jnp.float32) ** shard_levels(key_of[8], (LAYERS, HEADS), ((1, 4),), -0.2, 0.2), -1.0, 2.5),
        "skip_gain": jnp.clip(0.5 + 1.5 * jax.random.uniform(key_of[9], (LAYERS, HEADS), jnp.float32) ** shard_levels(key_of[9], (LAYERS, HEADS), ((1, 4),), -0.2, 0.2), 0.5, 2.0),
        "conv_taps": scatter_about(key_of[10], (LAYERS, CONV, 3, SSD_DIM), CONV ** -0.5, 2.5, ((3, 4),)),
        "gate_gain": jnp.clip(1.0 + 0.18 * jax.random.normal(key_of[11], (LAYERS, SSD_DIM), jnp.float32), 0.1, 1.9),
        "w_project": scatter_about(key_of[12], (LAYERS, SSD_DIM, D), SSD_DIM ** -0.5, 0.109375, ((1, 4), (2, 8))),
        "states": scatter_about(key_of[13], (LAYERS, BATCH, HEADS, HEAD_DIM * STATE), 0.5, 3.0, ((1, 8), (2, 4)), jnp.float32),
        "recent": scatter_about(key_of[14], (LAYERS, BATCH, CONV - 1, 3, SSD_DIM), 1.0, 6.0, ((1, 8), (4, 4))),
    }


EPS = 1e-06

def run_block(tokens_now, level, norm_gain, w_gate, w_value, w_inmap, w_readout, w_step, step_bias, decay_log, skip_gain, conv_taps, gate_gain, w_project, states, recent):
    tokens_f = tokens_now.astype(jnp.float32)
    scale_one = lax.rsqrt(lax.optimization_barrier(jnp.mean(tokens_f * tokens_f, axis=-1, keepdims=True)) + EPS)
    gained = (tokens_f * norm_gain[level][None, :]).astype(jnp.bfloat16)

    def project(weight):
        return scale_one * jnp.dot(gained, weight[level], preferred_element_type=jnp.float32)
    gate_pre = project(w_gate)
    step_raw = project(w_step)
    stacked = jnp.stack([project(w_value), project(w_inmap), project(w_readout)], axis=1).astype(jnp.bfloat16)
    window = jnp.concatenate([recent[level], stacked[:, None]], axis=1)
    taps_sum = lax.optimization_barrier(jnp.sum(window.astype(jnp.float32) * conv_taps[level].astype(jnp.float32)[None], axis=1))
    active = jax.nn.silu(taps_sum)
    rows = tokens_now.shape[0]
    x_value = active[:, 0].reshape(rows, HEADS, HEAD_DIM)
    in_map = active[:, 1].reshape(rows, HEADS, STATE)
    out_map = active[:, 2].reshape(rows, HEADS, STATE)
    step_size = jax.nn.softplus(step_raw + step_bias[level][None, :])
    decay_rate = jnp.exp(-step_size * jnp.exp(decay_log[level])[None, :])
    old_state = states[level].reshape(rows, HEADS, HEAD_DIM, STATE)
    fresh = decay_rate[:, :, None, None] * old_state + (step_size[:, :, None] * x_value)[:, :, :, None] * in_map[:, :, None, :]
    head_out = jnp.einsum('bhpn,bhn->bhp', fresh, out_map) + skip_gain[level][None, :, None] * x_value
    gated = (head_out.reshape(rows, SSD_DIM) * jax.nn.silu(gate_pre) * gate_gain[level][None, :]).astype(jnp.bfloat16)
    gated_f = gated.astype(jnp.float32)
    scale_two = lax.rsqrt(lax.optimization_barrier(jnp.mean(gated_f * gated_f, axis=-1, keepdims=True)) + EPS)
    mixed_out = scale_two * jnp.dot(gated, w_project[level], preferred_element_type=jnp.float32)
    return ((tokens_f + mixed_out).astype(jnp.bfloat16), fresh.reshape(rows, HEADS, HEAD_DIM * STATE), window[:, 1:])

def reference(tokens, norm_gain, w_gate, w_value, w_inmap, w_readout, w_step, step_bias, decay_log, skip_gain, conv_taps, gate_gain, w_project, states, recent):
    current = tokens
    state_list = []
    recent_list = []
    for level in range(LAYERS):
        current, fresh, kept = run_block(current, level, norm_gain, w_gate, w_value, w_inmap, w_readout, w_step, step_bias, decay_log, skip_gain, conv_taps, gate_gain, w_project, states, recent)
        state_list.append(fresh)
        recent_list.append(kept)
    return (current, jnp.stack(state_list, axis=0), jnp.stack(recent_list, axis=0))
```

```python
import functools

import jax
import jax.numpy as jnp
from jax import lax
from jax.experimental import pallas as pl
from jax.experimental.pallas import tpu as pltpu
from jax.sharding import PartitionSpec as P

EPS = 1e-06
LANES = 128
MESH = pl.DeviceIdType.MESH
F32 = jnp.float32
BF16 = jnp.bfloat16


def each(count, body):
    if count <= 8:
        for index in range(count):
            body(index)
    else:
        lax.fori_loop(0, count, lambda index, carry: (body(index), carry)[1], 0)


def fold(count, body, start):
    if count <= 8:
        for index in range(count):
            start = body(index, start)
        return start
    return lax.fori_loop(0, count, body, start)


def silu(value):
    return value / (1.0 + jnp.exp(-value))


def halves(value):
    high = value.astype(BF16)
    return high, (value - high.astype(F32)).astype(BF16)


def kernel(
    dims,
    tokens_ref,
    norm_ref,
    params_ref,
    conv_ref,
    value_hbm,
    inmap_hbm,
    readout_hbm,
    gate_hbm,
    step_hbm,
    project_hbm,
    states_hbm,
    tokens_out,
    fresh_hbm,
    u_out,
    w_in,
    w_step,
    w_out,
    state,
    spread,
    gather,
    part_send,
    part_recv,
    extra_send,
    extra_recv,
    gated_all,
    mixed_all,
    dec_ref,
    bm_ref,
    cm_ref,
    wide_ref,
    x_ref,
    in_sem,
    step_sem,
    out_sem,
    state_sem,
    fresh_sem,
    part_ssem,
    part_rsem,
    extra_ssem,
    extra_rsem,
    gated_ssem,
    gated_rsem,
    mixed_ssem,
    mixed_rsem,
):
    layers, dp, tp, own, cols, heads, head_dim, span, features, width = dims
    me = lax.axis_index("dp")
    col = lax.axis_index("tp")
    rows = dp * own

    def peer(k):
        return lax.rem(me + k + 1, dp)

    def column(k):
        return lax.rem(col + k + 1, tp)

    barrier = pltpu.get_barrier_semaphore()
    each(dp - 1, lambda k: pl.semaphore_signal(
        barrier, inc=1, device_id={"dp": peer(k)}, device_id_type=MESH))
    each(tp - 1, lambda k: pl.semaphore_signal(
        barrier, inc=1, device_id={"tp": column(k)}, device_id_type=MESH))

    sources = (inmap_hbm, readout_hbm, value_hbm, gate_hbm)

    def load_step(level):
        return pltpu.make_async_copy(step_hbm.at[level], w_step.at[level], step_sem.at[level])

    def load_in(level, w):
        return pltpu.make_async_copy(
            sources[w].at[level], w_in.at[level, w], in_sem.at[level, w])

    def load_out(level):
        return pltpu.make_async_copy(project_hbm.at[level], w_out.at[level], out_sem.at[level])

    def load_state(level):
        return pltpu.make_async_copy(states_hbm.at[level], state.at[level], state_sem.at[level])

    def save_state(level):
        return pltpu.make_async_copy(state.at[level], fresh_hbm.at[level], fresh_sem.at[level])

    for level in range(layers):
        load_step(level).start()
        for w in range(4):
            load_in(level, w).start()
        load_state(level).start()
        load_out(level).start()

    def send_extra(level, k):
        return pltpu.make_async_remote_copy(
            src_ref=extra_send.at[level, peer(k)],
            dst_ref=extra_recv.at[level, k],
            send_sem=extra_ssem.at[level, k],
            recv_sem=extra_rsem.at[level, k],
            device_id={"dp": peer(k)},
            device_id_type=MESH,
        )

    def send_part(level, w, k):
        return pltpu.make_async_remote_copy(
            src_ref=part_send.at[level, w, peer(k)],
            dst_ref=part_recv.at[level, w, k],
            send_sem=part_ssem.at[level, w, k],
            recv_sem=part_rsem.at[level, w, k],
            device_id={"dp": peer(k)},
            device_id_type=MESH,
        )

    def send_gated(level, k):
        return pltpu.make_async_remote_copy(
            src_ref=gated_all.at[level, me],
            dst_ref=gated_all.at[level, me],
            send_sem=gated_ssem.at[level, k],
            recv_sem=gated_rsem.at[level, k],
            device_id={"dp": peer(k)},
            device_id_type=MESH,
        )

    def send_mixed(level, k):
        return pltpu.make_async_remote_copy(
            src_ref=mixed_all.at[level, col],
            dst_ref=mixed_all.at[level, col],
            send_sem=mixed_ssem.at[level, k],
            recv_sem=mixed_rsem.at[level, k],
            device_id={"tp": column(k)},
            device_id_type=MESH,
        )

    x_ref[...] = tokens_ref[...].astype(F32)
    lane_all = lax.broadcasted_iota(jnp.int32, (rows, LANES), 1)
    lane = lax.broadcasted_iota(jnp.int32, (own, LANES), 1)
    low = lane < head_dim

    def twice(pair, odd):
        turned = pltpu.roll(pair, head_dim, 1)
        return jnp.where(low, turned, pair) if odd else jnp.where(low, pair, turned)

    for level in range(layers):
        x = x_ref[...]
        square = jnp.sum(x * x, axis=1, keepdims=True)
        gained = (x * norm_ref[level][None, :]).astype(BF16)
        load_step(level).wait()
        extra = jnp.dot(gained, w_step[level], preferred_element_type=F32)
        extra = jnp.where(lane_all == LANES - 1, square, extra).reshape(dp, own, LANES)
        high, rest = halves(extra)
        extra_send[level, :, :, :LANES] = high
        extra_send[level, :, :, LANES:] = rest
        if level == 0:
            pl.semaphore_wait(barrier, dp - 1 + tp - 1)
        each(dp - 1, lambda k: send_extra(level, k).start())
        for w in range(4):
            load_in(level, w).wait()
            part = jnp.dot(gained, w_in[level, w], preferred_element_type=F32)
            part_send[level, w] = part.reshape(dp, own, cols).astype(BF16)
            each(dp - 1, lambda k: send_part(level, w, k).start())

        if level == 0:
            step = 256

            def build(index, carry):
                start = pl.multiple_of(index * step, step)
                entry = lax.broadcasted_iota(jnp.int32, (LANES, step), 1) + start
                which = lax.broadcasted_iota(jnp.int32, (LANES, step), 0)
                spread[:, pl.ds(start, step)] = jnp.where(
                    lax.rem(which, head_dim) == entry // span, 1.0, 0.0).astype(BF16)
                entry = lax.broadcasted_iota(jnp.int32, (step, LANES), 0) + start
                which = lax.broadcasted_iota(jnp.int32, (step, LANES), 1)
                gather[pl.ds(start, step), :] = jnp.where(
                    lax.rem(which, head_dim) == entry // span, 1.0, 0.0).astype(BF16)
                return carry

            lax.fori_loop(0, head_dim * span // step, build, 0)

        each(dp - 1, lambda k: send_extra(level, k).wait_recv())

        def add_extra(k, total):
            return total + extra_recv[level, k].astype(F32)

        both = fold(dp - 1, add_extra, extra_send[level, me].astype(F32))
        total = both[:, :LANES] + both[:, LANES:]
        scale = lax.rsqrt(total[:, LANES - 1 :] / features + EPS)
        pick = lax.broadcasted_iota(jnp.int32, (LANES, cols), 0)
        slot = lax.broadcasted_iota(jnp.int32, (LANES, cols), 1)
        chosen = jnp.where(pick == col * heads + slot // head_dim, 1.0, 0.0).astype(BF16)
        high, rest = halves(total * scale)
        raw = jnp.dot(high, chosen, preferred_element_type=F32) + jnp.dot(
            rest, chosen, preferred_element_type=F32)
        raw = raw + params_ref[level, 0:1, :]
        size = jnp.maximum(raw, 0.0) + jnp.log1p(jnp.exp(-jnp.abs(raw)))
        decay = jnp.exp(-size * params_ref[level, 1:2, :])

        def total_part(w):
            each(dp - 1, lambda k: send_part(level, w, k).wait_recv())
            return scale * fold(
                dp - 1,
                lambda k, sum_in: sum_in + part_recv[level, w, k].astype(F32),
                part_send[level, w, me].astype(F32),
            )

        def active(w, place):
            u = total_part(w).astype(BF16)
            u_out[level, :, place * cols : (place + 1) * cols] = u
            return silu(
                conv_ref[level, :, place * cols : (place + 1) * cols]
                + u.astype(F32) * params_ref[level, 4 + place : 5 + place, :])

        bm = active(0, 1)
        cm = active(1, 2)
        for h in range(heads):
            window = slice(h // 2 * LANES, h // 2 * LANES + LANES)
            dec_ref[h] = twice(decay[:, window], h % 2)
            bm_ref[h] = twice(bm[:, window], h % 2)
            cm_ref[h] = twice(cm[:, window], h % 2)
        xv = active(2, 0)
        weighted = size * xv
        for h in range(heads):
            window = slice(h // 2 * LANES, h // 2 * LANES + LANES)
            one = twice(weighted[:, window], h % 2)
            high = one.astype(BF16).astype(F32)
            wide_ref[h * own : (h + 1) * own, :] = jnp.where(low, high, one - high)
        wide = wide_ref[...].astype(BF16)
        load_state(level).wait()
        piece = 512

        def advance(index, y):
            start = pl.multiple_of(index * piece, piece)
            window = pl.ds(start, piece)
            grown = jnp.dot(wide, spread[:, window], preferred_element_type=F32)
            read = []
            for h in range(heads):
                def across(ref):
                    return jnp.concatenate([ref[h]] * (piece // LANES), axis=1)

                fresh = across(dec_ref) * state[level, h, :, window] + (
                    grown[h * own : (h + 1) * own] * across(bm_ref))
                state[level, h, :, window] = fresh
                read.append(fresh * across(cm_ref))
            read = jnp.concatenate(read, axis=0).astype(BF16)
            return y + jnp.dot(read, gather[window, :], preferred_element_type=F32)

        y = lax.fori_loop(
            0, head_dim * span // piece, advance, jnp.zeros((heads * own, LANES), F32))
        save_state(level).start()
        y = jnp.concatenate(
            [
                jnp.where(low, y[h * own : (h + 1) * own], y[(h + 1) * own : (h + 2) * own])
                for h in range(0, heads, 2)
            ],
            axis=1,
        )
        y = y + params_ref[level, 2:3, :] * xv
        gate = total_part(3)
        gated_all[level, me] = (y * silu(gate) * params_ref[level, 3:4, :]).astype(BF16)
        each(dp - 1, lambda k: send_gated(level, k).start())
        load_out(level).wait()
        each(dp - 1, lambda k: send_gated(level, k).wait_recv())
        gated = gated_all[level].astype(F32).reshape(rows, cols)
        square = jnp.sum(gated * gated, axis=1, keepdims=True)
        mixed = jnp.dot(gated.astype(BF16), w_out[level], preferred_element_type=F32)
        high = square.astype(BF16).astype(F32)
        mixed_all[level, col, :, :width] = mixed.astype(BF16)
        mixed_all[level, col, :, width:] = jnp.where(
            lane_all < LANES // 2, high, square - high).astype(BF16)
        each(tp - 1, lambda k: send_mixed(level, k).start())
        each(tp - 1, lambda k: send_mixed(level, k).wait_recv())
        mixed = fold(
            tp,
            lambda k, sum_in: sum_in + mixed_all[level, k].astype(F32),
            jnp.zeros((rows, width + LANES), F32),
        )
        square = mixed[:, width : width + 1] + mixed[:, width + LANES - 1 :]
        scale = lax.rsqrt(square / (cols * tp) + EPS)
        fresh_x = (x_ref[...] + scale * mixed[:, :width]).astype(BF16)
        x_ref[...] = fresh_x.astype(F32)
        if level == layers - 1:
            tokens_out[...] = fresh_x

    for level in range(layers):
        save_state(level).wait()
        each(dp - 1, lambda k: send_extra(level, k).wait_send())
        for w in range(4):
            each(dp - 1, lambda k: send_part(level, w, k).wait_send())
        each(dp - 1, lambda k: send_gated(level, k).wait_send())
        each(tp - 1, lambda k: send_mixed(level, k).wait_send())


def per_device(
    dp,
    tp,
    tokens,
    norm_gain,
    w_gate,
    w_value,
    w_inmap,
    w_readout,
    w_step,
    step_bias,
    decay_log,
    skip_gain,
    conv_taps,
    gate_gain,
    w_project,
    states,
    recent,
):
    layers, own, heads, entries = states.shape
    cols = w_gate.shape[2]
    head_dim = cols // heads
    span = entries // head_dim
    width = tokens.shape[1]
    features = width * dp
    dims = (layers, dp, tp, own, cols, heads, head_dim, span, features, width)
    rows = tokens.shape[0]

    def expand(value):
        return jnp.repeat(value, head_dim, axis=1)[:, None]

    taps = conv_taps.astype(F32)
    params = jnp.concatenate(
        [
            expand(step_bias),
            expand(jnp.exp(decay_log)),
            expand(skip_gain),
            gate_gain[:, None],
            taps[:, -1],
        ],
        axis=1,
    )
    kept = jnp.sum(recent.astype(F32) * taps[:, None, :-1], axis=2).reshape(layers, own, 3 * cols)
    step_weight = jnp.pad(w_step, ((0, 0), (0, 0), (0, LANES - w_step.shape[2])))
    turned = states.transpose(0, 2, 1, 3)
    vmem = pl.BlockSpec(memory_space=pltpu.VMEM)
    anywhere = pl.BlockSpec(memory_space=pl.ANY)
    dma = pltpu.SemaphoreType.DMA
    out_tokens, fresh, u = pl.pallas_call(
        functools.partial(kernel, dims),
        out_shape=(
            jax.ShapeDtypeStruct((rows, width), BF16),
            jax.ShapeDtypeStruct((layers, heads, own, entries), F32),
            jax.ShapeDtypeStruct((layers, own, 3 * cols), BF16),
        ),
        in_specs=[vmem] * 4 + [anywhere] * 7,
        out_specs=(vmem, anywhere, vmem),
        scratch_shapes=[
            pltpu.VMEM((layers, 4, width, cols), BF16),
            pltpu.VMEM((layers, width, LANES), BF16),
            pltpu.VMEM((layers, cols, width), BF16),
            pltpu.VMEM((layers, heads, own, entries), F32),
            pltpu.VMEM((LANES, entries), BF16),
            pltpu.VMEM((entries, LANES), BF16),
            pltpu.VMEM((layers, 4, dp, own, cols), BF16),
            pltpu.VMEM((layers, 4, dp - 1, own, cols), BF16),
            pltpu.VMEM((layers, dp, own, 2 * LANES), BF16),
            pltpu.VMEM((layers, dp - 1, own, 2 * LANES), BF16),
            pltpu.VMEM((layers, dp, own, cols), BF16),
            pltpu.VMEM((layers, tp, rows, width + LANES), BF16),
            pltpu.VMEM((heads, own, LANES), F32),
            pltpu.VMEM((heads, own, LANES), F32),
            pltpu.VMEM((heads, own, LANES), F32),
            pltpu.VMEM((heads * own, LANES), F32),
            pltpu.VMEM((rows, width), F32),
            dma((layers, 4)),
            dma((layers,)),
            dma((layers,)),
            dma((layers,)),
            dma((layers,)),
            dma((layers, 4, dp - 1)),
            dma((layers, 4, dp - 1)),
            dma((layers, dp - 1)),
            dma((layers, dp - 1)),
            dma((layers, dp - 1)),
            dma((layers, dp - 1)),
            dma((layers, tp - 1)),
            dma((layers, tp - 1)),
        ],
        compiler_params=pltpu.CompilerParams(
            collective_id=0, has_side_effects=True, vmem_limit_bytes=50 * 1024 * 1024),
    )(
        tokens,
        norm_gain,
        params,
        kept,
        w_value,
        w_inmap,
        w_readout,
        w_gate,
        step_weight,
        w_project,
        turned,
    )
    next_states = fresh.transpose(0, 2, 1, 3)
    next_recent = jnp.concatenate(
        [recent[:, :, 1:], u.reshape(layers, own, 1, 3, cols)], axis=2)
    return out_tokens, next_states, next_recent


def solution(mesh):
    in_specs = (
        P(None, "dp"),
        P(None, "dp"),
        P(None, "dp", "tp"),
        P(None, "dp", "tp"),
        P(None, "dp", "tp"),
        P(None, "dp", "tp"),
        P(None, "dp", None),
        P(None, "tp"),
        P(None, "tp"),
        P(None, "tp"),
        P(None, None, None, "tp"),
        P(None, "tp"),
        P(None, "tp", "dp"),
        P(None, "dp", "tp", None),
        P(None, "dp", None, None, "tp"),
    )
    out_specs = (P(None, "dp"), P(None, "dp", "tp", None), P(None, "dp", None, None, "tp"))
    body = functools.partial(per_device, mesh.shape["dp"], mesh.shape["tp"])
    return jax.shard_map(
        body, mesh=mesh, in_specs=in_specs, out_specs=out_specs, check_vma=False
    )
```

```python
import functools

import jax
import jax.numpy as jnp
from jax import lax
from jax.experimental import pallas as pl
from jax.experimental.pallas import tpu as pltpu
from jax.sharding import PartitionSpec as P

EPS = 1e-06
LANES = 128
MESH = pl.DeviceIdType.MESH
F32 = jnp.float32
BF16 = jnp.bfloat16


def each(count, body):
    if count <= 8:
        for index in range(count):
            body(index)
    else:
        lax.fori_loop(0, count, lambda index, carry: (body(index), carry)[1], 0)


def fold(count, body, start):
    if count <= 8:
        for index in range(count):
            start = body(index, start)
        return start
    return lax.fori_loop(0, count, body, start)


def silu(value):
    return value / (1.0 + jnp.exp(-value))


def halves(value):
    high = value.astype(BF16)
    return high, (value - high.astype(F32)).astype(BF16)


def kernel(
    dims,
    tokens_ref,
    norm_ref,
    bias_ref,
    rate_ref,
    skip_ref,
    gain_ref,
    taps_ref,
    recent_ref,
    value_hbm,
    inmap_hbm,
    readout_hbm,
    gate_hbm,
    step_hbm,
    project_hbm,
    states_hbm,
    tokens_out,
    fresh_out,
    u_out,
    w_in,
    w_step,
    w_out,
    state,
    spread,
    gather,
    part_send,
    part_recv,
    extra_send,
    extra_recv,
    gated_all,
    mixed_all,
    square_all,
    conv_ref,
    params_ref,
    chosen_ref,
    dec_ref,
    bm_ref,
    cm_ref,
    wide_ref,
    x_ref,
    in_sem,
    step_sem,
    out_sem,
    state_sem,
    part_ssem,
    part_rsem,
    extra_ssem,
    extra_rsem,
    gated_ssem,
    gated_rsem,
    mixed_ssem,
    mixed_rsem,
    square_ssem,
    square_rsem,
):
    layers, dp, tp, own, cols, heads, head_dim, span, features, width = dims
    me = lax.axis_index("dp")
    col = lax.axis_index("tp")
    rows = dp * own

    def peer(k):
        return lax.rem(me + k + 1, dp)

    def column(k):
        return lax.rem(col + k + 1, tp)

    barrier = pltpu.get_barrier_semaphore()
    each(dp - 1, lambda k: pl.semaphore_signal(
        barrier, inc=1, device_id={"dp": peer(k)}, device_id_type=MESH))
    each(tp - 1, lambda k: pl.semaphore_signal(
        barrier, inc=1, device_id={"tp": column(k)}, device_id_type=MESH))

    sources = (inmap_hbm, readout_hbm, value_hbm, gate_hbm)

    def load_step(level):
        return pltpu.make_async_copy(step_hbm.at[level], w_step.at[level, : step_hbm.shape[1]], step_sem.at[level])

    def load_in(level, w):
        return pltpu.make_async_copy(
            sources[w].at[level], w_in.at[level, w], in_sem.at[level, w])

    def load_out(level):
        return pltpu.make_async_copy(project_hbm.at[level], w_out.at[level], out_sem.at[level])

    def load_state(level):
        return pltpu.make_async_copy(states_hbm.at[level], state.at[level], state_sem.at[level])

    filled = step_hbm.shape[1]
    w_step[:, filled:] = jnp.zeros((layers, LANES - filled, width), BF16)
    for level in range(layers):
        load_step(level).start()
        for w in range(4):
            load_in(level, w).start()
        load_state(level).start()
        load_out(level).start()

    def send_extra(level, k):
        return pltpu.make_async_remote_copy(
            src_ref=extra_send.at[level, peer(k)],
            dst_ref=extra_recv.at[level, k],
            send_sem=extra_ssem.at[level, k],
            recv_sem=extra_rsem.at[level, k],
            device_id={"dp": peer(k)},
            device_id_type=MESH,
        )

    def send_part(level, w, k):
        return pltpu.make_async_remote_copy(
            src_ref=part_send.at[level, w, peer(k)],
            dst_ref=part_recv.at[level, w, k],
            send_sem=part_ssem.at[level, w, k],
            recv_sem=part_rsem.at[level, w, k],
            device_id={"dp": peer(k)},
            device_id_type=MESH,
        )

    def send_gated(level, k):
        return pltpu.make_async_remote_copy(
            src_ref=gated_all.at[level, me],
            dst_ref=gated_all.at[level, me],
            send_sem=gated_ssem.at[level, k],
            recv_sem=gated_rsem.at[level, k],
            device_id={"dp": peer(k)},
            device_id_type=MESH,
        )

    def send_mixed(level, k):
        return pltpu.make_async_remote_copy(
            src_ref=mixed_all.at[level, col],
            dst_ref=mixed_all.at[level, col],
            send_sem=mixed_ssem.at[level, k],
            recv_sem=mixed_rsem.at[level, k],
            device_id={"tp": column(k)},
            device_id_type=MESH,
        )

    def send_square(level, k):
        return pltpu.make_async_remote_copy(
            src_ref=square_all.at[level, col],
            dst_ref=square_all.at[level, col],
            send_sem=square_ssem.at[level, k],
            recv_sem=square_rsem.at[level, k],
            device_id={"tp": column(k)},
            device_id_type=MESH,
        )

    x_ref[...] = tokens_ref[...].astype(F32)
    lane_all = lax.broadcasted_iota(jnp.int32, (rows, LANES), 1)
    lane = lax.broadcasted_iota(jnp.int32, (own, LANES), 1)
    low = lane < head_dim

    def twice(pair, odd):
        turned = pltpu.roll(pair, head_dim, 1)
        return jnp.where(low, turned, pair) if odd else jnp.where(low, pair, turned)

    for level in range(layers):
        x = x_ref[...]
        square = jnp.sum(x * x, axis=1, keepdims=True)
        gained = (x * norm_ref[level][None, :]).astype(BF16)
        load_step(level).wait()
        extra = lax.dot_general(
            gained, w_step[level], (((1,), (1,)), ((), ())), preferred_element_type=F32)
        extra = jnp.where(lane_all == LANES - 1, square, extra).reshape(dp, own, LANES)
        high, rest = halves(extra)
        extra_send[level, :, :, :LANES] = high
        extra_send[level, :, :, LANES:] = rest
        if level == 0:
            pl.semaphore_wait(barrier, dp - 1 + tp - 1)
        each(dp - 1, lambda k: send_extra(level, k).start())
        for w in range(4):
            load_in(level, w).wait()
            part = jnp.dot(gained, w_in[level, w], preferred_element_type=F32)
            part_send[level, w] = part.reshape(dp, own, cols).astype(BF16)
            each(dp - 1, lambda k: send_part(level, w, k).start())

        if level == 0:
            step = 256

            def build(index, carry):
                start = pl.multiple_of(index * step, step)
                entry = lax.broadcasted_iota(jnp.int32, (LANES, step), 1) + start
                which = lax.broadcasted_iota(jnp.int32, (LANES, step), 0)
                spread[:, pl.ds(start, step)] = jnp.where(
                    lax.rem(which, head_dim) == entry // span, 1.0, 0.0).astype(BF16)
                entry = lax.broadcasted_iota(jnp.int32, (step, LANES), 0) + start
                which = lax.broadcasted_iota(jnp.int32, (step, LANES), 1)
                gather[pl.ds(start, step), :] = jnp.where(
                    lax.rem(which, head_dim) == entry // span, 1.0, 0.0).astype(BF16)
                return carry

            lax.fori_loop(0, head_dim * span // step, build, 0)
            pick = lax.broadcasted_iota(jnp.int32, (LANES, cols), 0)
            slot = lax.broadcasted_iota(jnp.int32, (LANES, cols), 1)
            chosen_ref[...] = jnp.where(
                pick == col * heads + slot // head_dim, 1.0, 0.0).astype(BF16)
            pick = lax.broadcasted_iota(jnp.int32, (heads, cols), 0)
            slot = lax.broadcasted_iota(jnp.int32, (heads, cols), 1)
            wider = jnp.where(pick == slot // head_dim, 1.0, 0.0)
            for place, value in enumerate((bias_ref[...], jnp.exp(rate_ref[...]), skip_ref[...])):
                params_ref[place] = jnp.dot(
                    value, wider, preferred_element_type=F32, precision=lax.Precision.HIGHEST)

        def convolve(j):
            return jnp.sum(
                recent_ref[level, :, j].astype(F32)
                * taps_ref[: taps_ref.shape[0] - 1, j, level, :].astype(F32)[None],
                axis=1,
            )

        for j in range(3):
            conv_ref[j] = convolve(j)

        each(dp - 1, lambda k: send_extra(level, k).wait_recv())

        def add_extra(k, total):
            return total + extra_recv[level, k].astype(F32)

        both = fold(dp - 1, add_extra, extra_send[level, me].astype(F32))
        total = both[:, :LANES] + both[:, LANES:]
        scale = lax.rsqrt(total[:, LANES - 1 :] / features + EPS)
        chosen = chosen_ref[...]
        high, rest = halves(total * scale)
        raw = jnp.dot(high, chosen, preferred_element_type=F32) + jnp.dot(
            rest, chosen, preferred_element_type=F32)
        raw = raw + params_ref[0, level : level + 1, :]
        size = jnp.maximum(raw, 0.0) + jnp.log1p(jnp.exp(-jnp.abs(raw)))
        decay = jnp.exp(-size * params_ref[1, level : level + 1, :])

        def total_part(w):
            each(dp - 1, lambda k: send_part(level, w, k).wait_recv())
            return scale * fold(
                dp - 1,
                lambda k, sum_in: sum_in + part_recv[level, w, k].astype(F32),
                part_send[level, w, me].astype(F32),
            )

        def active(w, place):
            u = total_part(w).astype(BF16)
            u_out[level, :, place * cols : (place + 1) * cols] = u
            return silu(
                conv_ref[place]
                + u.astype(F32) * taps_ref[taps_ref.shape[0] - 1, place, level : level + 1, :].astype(F32))

        bm = active(0, 1)
        cm = active(1, 2)
        for h in range(heads):
            window = slice(h // 2 * LANES, h // 2 * LANES + LANES)
            dec_ref[h] = twice(decay[:, window], h % 2)
            bm_ref[h] = twice(bm[:, window], h % 2)
            cm_ref[h] = twice(cm[:, window], h % 2)
        load_state(level).wait()
        piece = 512
        pieces = head_dim * span // piece

        def across(ref, h):
            return jnp.concatenate([ref[h]] * (piece // LANES), axis=1)

        def consult(index, y):
            window = pl.ds(pl.multiple_of(index * piece, piece), piece)
            read = jnp.concatenate(
                [state[level, h, :, window] * across(cm_ref, h) for h in range(heads)], axis=0)
            return y + jnp.dot(
                read.astype(BF16), gather[window, :], preferred_element_type=F32)

        y = lax.fori_loop(0, pieces, consult, jnp.zeros((heads * own, LANES), F32))
        xv = active(2, 0)
        weighted = size * xv
        inner = []
        for h in range(heads):
            window = slice(h // 2 * LANES, h // 2 * LANES + LANES)
            one = twice(weighted[:, window], h % 2)
            high = one.astype(BF16).astype(F32)
            wide_ref[h * own : (h + 1) * own, :] = jnp.where(low, high, one - high)
            within = jnp.sum(
                jnp.where(low, bm_ref[h] * cm_ref[h], 0.0), axis=1, keepdims=True)
            inner.append(dec_ref[h] * y[h * own : (h + 1) * own] + one * within)
        y = jnp.concatenate(
            [jnp.where(low, inner[h], inner[h + 1]) for h in range(0, heads, 2)], axis=1)
        y = y + params_ref[2, level : level + 1, :] * xv
        gate = total_part(3)
        gated_all[level, me] = (y * silu(gate) * gain_ref[level : level + 1, :]).astype(BF16)
        each(dp - 1, lambda k: send_gated(level, k).start())
        wide = wide_ref[...].astype(BF16)

        def advance(index, carry):
            window = pl.ds(pl.multiple_of(index * piece, piece), piece)
            grown = jnp.dot(wide, spread[:, window], preferred_element_type=F32)
            for h in range(heads):
                fresh_out[level, h, :, window] = (
                    across(dec_ref, h) * state[level, h, :, window]
                    + grown[h * own : (h + 1) * own] * across(bm_ref, h))
            return carry

        lax.fori_loop(0, pieces, advance, 0)
        load_out(level).wait()
        each(dp - 1, lambda k: send_gated(level, k).wait_recv())
        gated = gated_all[level].astype(F32).reshape(rows, cols)
        square = jnp.sum(gated * gated, axis=1, keepdims=True)
        mixed = jnp.dot(gated.astype(BF16), w_out[level], preferred_element_type=F32)
        mixed_all[level, col] = mixed.astype(BF16)
        each(tp - 1, lambda k: send_mixed(level, k).start())
        cross = lax.broadcasted_iota(jnp.int32, (rows, rows), 0) == (
            lax.broadcasted_iota(jnp.int32, (rows, rows), 1))
        square_all[level, col, :, :rows] = jnp.broadcast_to(
            jnp.sum(jnp.where(cross, square, 0.0), axis=0, keepdims=True), (8, rows))
        each(tp - 1, lambda k: send_square(level, k).start())
        each(tp - 1, lambda k: send_square(level, k).wait_recv())
        square = fold(
            tp,
            lambda k, sum_in: sum_in + square_all[level, k, 0:1, :rows],
            jnp.zeros((1, rows), F32),
        )
        scale = lax.rsqrt(square / (cols * tp) + EPS)
        scale = jnp.sum(jnp.where(cross, scale, 0.0), axis=1, keepdims=True)
        each(tp - 1, lambda k: send_mixed(level, k).wait_recv())
        mixed = fold(
            tp,
            lambda k, sum_in: sum_in + mixed_all[level, k].astype(F32),
            jnp.zeros((rows, width), F32),
        )
        fresh_x = (x_ref[...] + scale * mixed).astype(BF16)
        x_ref[...] = fresh_x.astype(F32)
        if level == layers - 1:
            tokens_out[...] = fresh_x

    for level in range(layers):
        each(dp - 1, lambda k: send_extra(level, k).wait_send())
        for w in range(4):
            each(dp - 1, lambda k: send_part(level, w, k).wait_send())
        each(dp - 1, lambda k: send_gated(level, k).wait_send())
        each(tp - 1, lambda k: send_mixed(level, k).wait_send())
        each(tp - 1, lambda k: send_square(level, k).wait_send())


def per_device(
    dp,
    tp,
    tokens,
    norm_gain,
    w_gate,
    w_value,
    w_inmap,
    w_readout,
    w_step,
    step_bias,
    decay_log,
    skip_gain,
    conv_taps,
    gate_gain,
    w_project,
    states,
    recent,
):
    layers, own, heads, entries = states.shape
    cols = w_gate.shape[2]
    head_dim = cols // heads
    span = entries // head_dim
    width = tokens.shape[1]
    features = width * dp
    dims = (layers, dp, tp, own, cols, heads, head_dim, span, features, width)
    rows = tokens.shape[0]

    vmem = pl.BlockSpec(memory_space=pltpu.VMEM)
    anywhere = pl.BlockSpec(memory_space=pl.ANY)
    dma = pltpu.SemaphoreType.DMA
    out_tokens, fresh, u = pl.pallas_call(
        functools.partial(kernel, dims),
        out_shape=(
            jax.ShapeDtypeStruct((rows, width), BF16),
            jax.ShapeDtypeStruct((layers, heads, own, entries), F32),
            jax.ShapeDtypeStruct((layers, own, 3 * cols), BF16),
        ),
        in_specs=[vmem] * 8 + [anywhere] * 7,
        out_specs=(vmem, vmem, vmem),
        scratch_shapes=[
            pltpu.VMEM((layers, 4, width, cols), BF16),
            pltpu.VMEM((layers, LANES, width), BF16),
            pltpu.VMEM((layers, cols, width), BF16),
            pltpu.VMEM((layers, heads, own, entries), F32),
            pltpu.VMEM((LANES, entries), BF16),
            pltpu.VMEM((entries, LANES), BF16),
            pltpu.VMEM((layers, 4, dp, own, cols), BF16),
            pltpu.VMEM((layers, 4, dp - 1, own, cols), BF16),
            pltpu.VMEM((layers, dp, own, 2 * LANES), BF16),
            pltpu.VMEM((layers, dp - 1, own, 2 * LANES), BF16),
            pltpu.VMEM((layers, dp, own, cols), BF16),
            pltpu.VMEM((layers, tp, rows, width), BF16),
            pltpu.VMEM((layers, tp, 8, -(-rows // LANES) * LANES), F32),
            pltpu.VMEM((3, own, cols), F32),
            pltpu.VMEM((3, layers, cols), F32),
            pltpu.VMEM((LANES, cols), BF16),
            pltpu.VMEM((heads, own, LANES), F32),
            pltpu.VMEM((heads, own, LANES), F32),
            pltpu.VMEM((heads, own, LANES), F32),
            pltpu.VMEM((heads * own, LANES), F32),
            pltpu.VMEM((rows, width), F32),
            dma((layers, 4)),
            dma((layers,)),
            dma((layers,)),
            dma((layers,)),
            dma((layers, 4, dp - 1)),
            dma((layers, 4, dp - 1)),
            dma((layers, dp - 1)),
            dma((layers, dp - 1)),
            dma((layers, dp - 1)),
            dma((layers, dp - 1)),
            dma((layers, tp - 1)),
            dma((layers, tp - 1)),
            dma((layers, tp - 1)),
            dma((layers, tp - 1)),
        ],
        compiler_params=pltpu.CompilerParams(
            collective_id=0, has_side_effects=True, vmem_limit_bytes=60 * 1024 * 1024),
    )(
        tokens,
        norm_gain,
        step_bias,
        decay_log,
        skip_gain,
        gate_gain,
        conv_taps.transpose(1, 2, 0, 3),
        recent.transpose(0, 1, 3, 2, 4),
        w_value,
        w_inmap,
        w_readout,
        w_gate,
        w_step.transpose(0, 2, 1),
        w_project,
        states.transpose(0, 2, 1, 3),
    )
    next_states = fresh.transpose(0, 2, 1, 3)
    next_recent = jnp.concatenate(
        [recent[:, :, 1:], u.reshape(layers, own, 1, 3, cols)], axis=2)
    return out_tokens, next_states, next_recent


def solution(mesh):
    in_specs = (
        P(None, "dp"),
        P(None, "dp"),
        P(None, "dp", "tp"),
        P(None, "dp", "tp"),
        P(None, "dp", "tp"),
        P(None, "dp", "tp"),
        P(None, "dp", None),
        P(None, "tp"),
        P(None, "tp"),
        P(None, "tp"),
        P(None, None, None, "tp"),
        P(None, "tp"),
        P(None, "tp", "dp"),
        P(None, "dp", "tp", None),
        P(None, "dp", None, None, "tp"),
    )
    out_specs = (P(None, "dp"), P(None, "dp", "tp", None), P(None, "dp", None, None, "tp"))
    body = functools.partial(per_device, mesh.shape["dp"], mesh.shape["tp"])
    return jax.shard_map(
        body, mesh=mesh, in_specs=in_specs, out_specs=out_specs, check_vma=False
    )
```

```python
import functools

import jax
import jax.numpy as jnp
from jax import lax
from jax.experimental import pallas as pl
from jax.experimental.pallas import tpu as pltpu
from jax.sharding import PartitionSpec as P

EPS = 1e-06
LANES = 128
MESH = pl.DeviceIdType.MESH
F32 = jnp.float32
BF16 = jnp.bfloat16


def each(count, body):
    if count <= 8:
        for index in range(count):
            body(index)
    else:
        lax.fori_loop(0, count, lambda index, carry: (body(index), carry)[1], 0)


def fold(count, body, start):
    if count <= 8:
        for index in range(count):
            start = body(index, start)
        return start
    return lax.fori_loop(0, count, body, start)


def silu(value):
    return value / (1.0 + jnp.exp(-value))


def halves(value):
    high = value.astype(BF16)
    return high, (value - high.astype(F32)).astype(BF16)


def kernel(
    dims,
    tokens_ref,
    norm_ref,
    bias_ref,
    rate_ref,
    skip_ref,
    gain_ref,
    taps_ref,
    recent_ref,
    value_hbm,
    inmap_hbm,
    readout_hbm,
    gate_hbm,
    step_hbm,
    project_hbm,
    states_hbm,
    tokens_out,
    fresh_out,
    u_out,
    w_in,
    w_step,
    w_out,
    state,
    spread,
    gather,
    part_send,
    part_recv,
    extra_send,
    extra_recv,
    gated_all,
    mixed_all,
    square_all,
    conv_ref,
    params_ref,
    chosen_ref,
    dec_ref,
    bm_ref,
    cm_ref,
    wide_ref,
    x_ref,
    in_sem,
    step_sem,
    out_sem,
    state_sem,
    part_ssem,
    part_rsem,
    extra_ssem,
    extra_rsem,
    gated_ssem,
    gated_rsem,
    mixed_ssem,
    mixed_rsem,
    square_ssem,
    square_rsem,
):
    layers, dp, tp, own, cols, heads, head_dim, span, features, width = dims
    me = lax.axis_index("dp")
    col = lax.axis_index("tp")
    rows = dp * own

    def peer(k):
        return lax.rem(me + k + 1, dp)

    def column(k):
        return lax.rem(col + k + 1, tp)

    barrier = pltpu.get_barrier_semaphore()
    each(dp - 1, lambda k: pl.semaphore_signal(
        barrier, inc=1, device_id={"dp": peer(k)}, device_id_type=MESH))
    each(tp - 1, lambda k: pl.semaphore_signal(
        barrier, inc=1, device_id={"tp": column(k)}, device_id_type=MESH))

    sources = (inmap_hbm, readout_hbm, value_hbm, gate_hbm)

    def load_step(level):
        return pltpu.make_async_copy(step_hbm.at[level], w_step.at[level, : step_hbm.shape[1]], step_sem.at[level])

    def load_in(level, w):
        return pltpu.make_async_copy(
            sources[w].at[level], w_in.at[level, w], in_sem.at[level, w])

    def load_out(level):
        return pltpu.make_async_copy(project_hbm.at[level], w_out.at[level], out_sem.at[level])

    def load_state(level):
        return pltpu.make_async_copy(states_hbm.at[level], state.at[level], state_sem.at[level])

    filled = step_hbm.shape[1]
    w_step[:, filled:] = jnp.zeros((layers, LANES - filled, width), BF16)
    for level in range(layers):
        load_step(level).start()
        for w in range(4):
            load_in(level, w).start()
        load_state(level).start()
        load_out(level).start()

    def send_extra(level, k):
        return pltpu.make_async_remote_copy(
            src_ref=extra_send.at[level, peer(k)],
            dst_ref=extra_recv.at[level, k],
            send_sem=extra_ssem.at[level, k],
            recv_sem=extra_rsem.at[level, k],
            device_id={"dp": peer(k)},
            device_id_type=MESH,
        )

    def send_part(level, w, k):
        return pltpu.make_async_remote_copy(
            src_ref=part_send.at[level, w, peer(k)],
            dst_ref=part_recv.at[level, w, k],
            send_sem=part_ssem.at[level, w, k],
            recv_sem=part_rsem.at[level, w, k],
            device_id={"dp": peer(k)},
            device_id_type=MESH,
        )

    def send_gated(level, k):
        return pltpu.make_async_remote_copy(
            src_ref=gated_all.at[level, me],
            dst_ref=gated_all.at[level, me],
            send_sem=gated_ssem.at[level, k],
            recv_sem=gated_rsem.at[level, k],
            device_id={"dp": peer(k)},
            device_id_type=MESH,
        )

    def send_mixed(level, k):
        return pltpu.make_async_remote_copy(
            src_ref=mixed_all.at[level, col],
            dst_ref=mixed_all.at[level, col],
            send_sem=mixed_ssem.at[level, k],
            recv_sem=mixed_rsem.at[level, k],
            device_id={"tp": column(k)},
            device_id_type=MESH,
        )

    def send_square(level, k):
        return pltpu.make_async_remote_copy(
            src_ref=square_all.at[level, col],
            dst_ref=square_all.at[level, col],
            send_sem=square_ssem.at[level, k],
            recv_sem=square_rsem.at[level, k],
            device_id={"tp": column(k)},
            device_id_type=MESH,
        )

    x_ref[...] = tokens_ref[...].astype(F32)
    lane_all = lax.broadcasted_iota(jnp.int32, (rows, LANES), 1)
    lane = lax.broadcasted_iota(jnp.int32, (own, LANES), 1)
    low = lane < head_dim

    def twice(pair, odd):
        turned = pltpu.roll(pair, head_dim, 1)
        return jnp.where(low, turned, pair) if odd else jnp.where(low, pair, turned)

    for level in range(layers):
        x = x_ref[...]
        square = jnp.sum(x * x, axis=1, keepdims=True)
        gained = (x * norm_ref[level][None, :]).astype(BF16)
        load_step(level).wait()
        extra = lax.dot_general(
            gained, w_step[level], (((1,), (1,)), ((), ())), preferred_element_type=F32)
        extra = jnp.where(lane_all == LANES - 1, square, extra).reshape(dp, own, LANES)
        high, rest = halves(extra)
        extra_send[level, :, :, :LANES] = high
        extra_send[level, :, :, LANES:] = rest
        if level == 0:
            pl.semaphore_wait(barrier, dp - 1 + tp - 1)
        each(dp - 1, lambda k: send_extra(level, k).start())
        for w in range(4):
            load_in(level, w).wait()
            part = jnp.dot(gained, w_in[level, w], preferred_element_type=F32)
            part_send[level, w] = part.reshape(dp, own, cols).astype(BF16)
            each(dp - 1, lambda k: send_part(level, w, k).start())

        if level == 0:
            step = 256

            def build(index, carry):
                start = pl.multiple_of(index * step, step)
                entry = lax.broadcasted_iota(jnp.int32, (LANES, step), 1) + start
                which = lax.broadcasted_iota(jnp.int32, (LANES, step), 0)
                spread[:, pl.ds(start, step)] = jnp.where(
                    lax.rem(which, head_dim) == entry // span, 1.0, 0.0).astype(BF16)
                entry = lax.broadcasted_iota(jnp.int32, (step, LANES), 0) + start
                which = lax.broadcasted_iota(jnp.int32, (step, LANES), 1)
                gather[pl.ds(start, step), :] = jnp.where(
                    lax.rem(which, head_dim) == entry // span, 1.0, 0.0).astype(BF16)
                return carry

            lax.fori_loop(0, head_dim * span // step, build, 0)
            pick = lax.broadcasted_iota(jnp.int32, (LANES, cols), 0)
            slot = lax.broadcasted_iota(jnp.int32, (LANES, cols), 1)
            chosen_ref[...] = jnp.where(
                pick == col * heads + slot // head_dim, 1.0, 0.0).astype(BF16)
            pick = lax.broadcasted_iota(jnp.int32, (heads, cols), 0)
            slot = lax.broadcasted_iota(jnp.int32, (heads, cols), 1)
            wider = jnp.where(pick == slot // head_dim, 1.0, 0.0)
            for place, value in enumerate((bias_ref[...], jnp.exp(rate_ref[...]), skip_ref[...])):
                params_ref[place] = jnp.dot(
                    value, wider, preferred_element_type=F32, precision=lax.Precision.HIGHEST)

        def convolve(j):
            return jnp.sum(
                recent_ref[level, :, j].astype(F32)
                * taps_ref[: taps_ref.shape[0] - 1, j, level, :].astype(F32)[None],
                axis=1,
            )

        for j in range(3):
            conv_ref[j] = convolve(j)

        each(dp - 1, lambda k: send_extra(level, k).wait_recv())

        def add_extra(k, total):
            return total + extra_recv[level, k].astype(F32)

        both = fold(dp - 1, add_extra, extra_send[level, me].astype(F32))
        total = both[:, :LANES] + both[:, LANES:]
        scale = lax.rsqrt(total[:, LANES - 1 :] / features + EPS)
        chosen = chosen_ref[...]
        high, rest = halves(total * scale)
        raw = jnp.dot(high, chosen, preferred_element_type=F32) + jnp.dot(
            rest, chosen, preferred_element_type=F32)
        raw = raw + params_ref[0, level : level + 1, :]
        size = jnp.maximum(raw, 0.0) + jnp.log1p(jnp.exp(-jnp.abs(raw)))
        decay = jnp.exp(-size * params_ref[1, level : level + 1, :])

        def total_part(w):
            each(dp - 1, lambda k: send_part(level, w, k).wait_recv())
            return scale * fold(
                dp - 1,
                lambda k, sum_in: sum_in + part_recv[level, w, k].astype(F32),
                part_send[level, w, me].astype(F32),
            )

        def active(w, place):
            u = total_part(w).astype(BF16)
            u_out[level, :, place * cols : (place + 1) * cols] = u
            return silu(
                conv_ref[place]
                + u.astype(F32) * taps_ref[taps_ref.shape[0] - 1, place, level : level + 1, :].astype(F32))

        bm = active(0, 1)
        cm = active(1, 2)
        for h in range(heads):
            window = slice(h // 2 * LANES, h // 2 * LANES + LANES)
            dec_ref[h] = twice(decay[:, window], h % 2)
            bm_ref[h] = twice(bm[:, window], h % 2)
            cm_ref[h] = twice(cm[:, window], h % 2)
        load_state(level).wait()
        piece = 512
        pieces = head_dim * span // piece

        def across(ref, h):
            return jnp.concatenate([ref[h]] * (piece // LANES), axis=1)

        def consult(index, y):
            window = pl.ds(pl.multiple_of(index * piece, piece), piece)
            read = jnp.concatenate(
                [state[level, h, :, window] * across(cm_ref, h) for h in range(heads)], axis=0)
            return y + jnp.dot(
                read.astype(BF16), gather[window, :], preferred_element_type=F32)

        y = lax.fori_loop(0, pieces, consult, jnp.zeros((heads * own, LANES), F32))
        xv = active(2, 0)
        weighted = size * xv
        inner = []
        for h in range(heads):
            window = slice(h // 2 * LANES, h // 2 * LANES + LANES)
            one = twice(weighted[:, window], h % 2)
            high = one.astype(BF16).astype(F32)
            wide_ref[h * own : (h + 1) * own, :] = jnp.where(low, high, one - high)
            within = jnp.sum(
                jnp.where(low, bm_ref[h] * cm_ref[h], 0.0), axis=1, keepdims=True)
            inner.append(dec_ref[h] * y[h * own : (h + 1) * own] + one * within)
        y = jnp.concatenate(
            [jnp.where(low, inner[h], inner[h + 1]) for h in range(0, heads, 2)], axis=1)
        y = y + params_ref[2, level : level + 1, :] * xv
        gate = total_part(3)
        gated_all[level, me] = (y * silu(gate) * gain_ref[level : level + 1, :]).astype(BF16)
        each(dp - 1, lambda k: send_gated(level, k).start())
        wide = wide_ref[...].astype(BF16)

        def advance(index, carry):
            window = pl.ds(pl.multiple_of(index * piece, piece), piece)
            grown = jnp.dot(wide, spread[:, window], preferred_element_type=F32)
            for h in range(heads):
                fresh_out[level, h, :, window] = (
                    across(dec_ref, h) * state[level, h, :, window]
                    + grown[h * own : (h + 1) * own] * across(bm_ref, h))
            return carry

        lax.fori_loop(0, pieces, advance, 0)
        load_out(level).wait()
        each(dp - 1, lambda k: send_gated(level, k).wait_recv())
        gated = gated_all[level].astype(F32).reshape(rows, cols)
        square = jnp.sum(gated * gated, axis=1, keepdims=True)
        mixed = jnp.dot(gated.astype(BF16), w_out[level], preferred_element_type=F32)
        mixed_all[level, col] = mixed.astype(BF16)
        each(tp - 1, lambda k: send_mixed(level, k).start())
        cross = lax.broadcasted_iota(jnp.int32, (rows, rows), 0) == (
            lax.broadcasted_iota(jnp.int32, (rows, rows), 1))
        square_all[level, col, :, :rows] = jnp.broadcast_to(
            jnp.sum(jnp.where(cross, square, 0.0), axis=0, keepdims=True), (8, rows))
        each(tp - 1, lambda k: send_square(level, k).start())
        each(tp - 1, lambda k: send_square(level, k).wait_recv())
        square = fold(
            tp,
            lambda k, sum_in: sum_in + square_all[level, k, 0:1, :rows],
            jnp.zeros((1, rows), F32),
        )
        scale = lax.rsqrt(square / (cols * tp) + EPS)
        scale = jnp.sum(jnp.where(cross, scale, 0.0), axis=1, keepdims=True)
        each(tp - 1, lambda k: send_mixed(level, k).wait_recv())
        mixed = fold(
            tp,
            lambda k, sum_in: sum_in + mixed_all[level, k].astype(F32),
            jnp.zeros((rows, width), F32),
        )
        fresh_x = (x_ref[...] + scale * mixed).astype(BF16)
        x_ref[...] = fresh_x.astype(F32)
        if level == layers - 1:
            tokens_out[...] = fresh_x

    for level in range(layers):
        each(dp - 1, lambda k: send_extra(level, k).wait_send())
        for w in range(4):
            each(dp - 1, lambda k: send_part(level, w, k).wait_send())
        each(dp - 1, lambda k: send_gated(level, k).wait_send())
        each(tp - 1, lambda k: send_mixed(level, k).wait_send())
        each(tp - 1, lambda k: send_square(level, k).wait_send())


def finish(
    fresh_ref, tokens_ref, u_ref, recent_ref, tokens_out, fresh_hbm, recent_out, fresh_sem
):
    layers, heads = fresh_ref.shape[:2]
    cols = recent_ref.shape[-1]

    def save(level, h):
        return pltpu.make_async_copy(
            fresh_ref.at[level, h], fresh_hbm.at[level, h], fresh_sem.at[level, h])

    for level in range(layers):
        for h in range(heads):
            save(level, h).start()
    tokens_out[...] = tokens_ref[...]
    for level in range(layers):
        for j in range(3):
            kept = recent_ref[level, :, j].astype(F32)
            u = u_ref[level, :, j * cols : (j + 1) * cols].astype(F32)
            recent_out[level, :, j] = jnp.concatenate(
                [kept[:, 1:], u[:, None]], axis=1).astype(BF16)
    for level in range(layers):
        for h in range(heads):
            save(level, h).wait()


def per_device(
    dp,
    tp,
    tokens,
    norm_gain,
    w_gate,
    w_value,
    w_inmap,
    w_readout,
    w_step,
    step_bias,
    decay_log,
    skip_gain,
    conv_taps,
    gate_gain,
    w_project,
    states,
    recent,
):
    layers, own, heads, entries = states.shape
    cols = w_gate.shape[2]
    head_dim = cols // heads
    span = entries // head_dim
    width = tokens.shape[1]
    features = width * dp
    dims = (layers, dp, tp, own, cols, heads, head_dim, span, features, width)
    rows = tokens.shape[0]

    vmem = pl.BlockSpec(memory_space=pltpu.VMEM)
    anywhere = pl.BlockSpec(memory_space=pltpu.HBM)
    turned = recent.transpose(0, 1, 3, 2, 4)
    dma = pltpu.SemaphoreType.DMA
    out_tokens, fresh, u = pl.pallas_call(
        functools.partial(kernel, dims),
        out_shape=(
            jax.ShapeDtypeStruct((rows, width), BF16),
            pltpu.VMEM((layers, heads, own, entries), F32),
            jax.ShapeDtypeStruct((layers, own, 3 * cols), BF16),
        ),
        in_specs=[vmem] * 8 + [anywhere] * 7,
        out_specs=(vmem, vmem, vmem),
        scratch_shapes=[
            pltpu.VMEM((layers, 4, width, cols), BF16),
            pltpu.VMEM((layers, LANES, width), BF16),
            pltpu.VMEM((layers, cols, width), BF16),
            pltpu.VMEM((layers, heads, own, entries), F32),
            pltpu.VMEM((LANES, entries), BF16),
            pltpu.VMEM((entries, LANES), BF16),
            pltpu.VMEM((layers, 4, dp, own, cols), BF16),
            pltpu.VMEM((layers, 4, dp - 1, own, cols), BF16),
            pltpu.VMEM((layers, dp, own, 2 * LANES), BF16),
            pltpu.VMEM((layers, dp - 1, own, 2 * LANES), BF16),
            pltpu.VMEM((layers, dp, own, cols), BF16),
            pltpu.VMEM((layers, tp, rows, width), BF16),
            pltpu.VMEM((layers, tp, 8, -(-rows // LANES) * LANES), F32),
            pltpu.VMEM((3, own, cols), F32),
            pltpu.VMEM((3, layers, cols), F32),
            pltpu.VMEM((LANES, cols), BF16),
            pltpu.VMEM((heads, own, LANES), F32),
            pltpu.VMEM((heads, own, LANES), F32),
            pltpu.VMEM((heads, own, LANES), F32),
            pltpu.VMEM((heads * own, LANES), F32),
            pltpu.VMEM((rows, width), F32),
            dma((layers, 4)),
            dma((layers,)),
            dma((layers,)),
            dma((layers,)),
            dma((layers, 4, dp - 1)),
            dma((layers, 4, dp - 1)),
            dma((layers, dp - 1)),
            dma((layers, dp - 1)),
            dma((layers, dp - 1)),
            dma((layers, dp - 1)),
            dma((layers, tp - 1)),
            dma((layers, tp - 1)),
            dma((layers, tp - 1)),
            dma((layers, tp - 1)),
        ],
        compiler_params=pltpu.CompilerParams(
            collective_id=0, has_side_effects=True, vmem_limit_bytes=56 * 1024 * 1024),
    )(
        tokens,
        norm_gain,
        step_bias,
        decay_log,
        skip_gain,
        gate_gain,
        conv_taps.transpose(1, 2, 0, 3),
        turned,
        w_value,
        w_inmap,
        w_readout,
        w_gate,
        w_step.transpose(0, 2, 1),
        w_project,
        states.transpose(0, 2, 1, 3),
    )
    out_tokens, fresh, kept = pl.pallas_call(
        finish,
        out_shape=(
            jax.ShapeDtypeStruct(out_tokens.shape, BF16),
            jax.ShapeDtypeStruct(fresh.shape, F32),
            jax.ShapeDtypeStruct(turned.shape, BF16),
        ),
        in_specs=[vmem] * 4,
        out_specs=(vmem, anywhere, vmem),
        scratch_shapes=[dma((layers, heads))],
        compiler_params=pltpu.CompilerParams(vmem_limit_bytes=16 * 1024 * 1024),
    )(fresh, out_tokens, u, turned)
    next_states = fresh.transpose(0, 2, 1, 3)
    next_recent = kept.transpose(0, 1, 3, 2, 4)
    return out_tokens, next_states, next_recent


def solution(mesh):
    in_specs = (
        P(None, "dp"),
        P(None, "dp"),
        P(None, "dp", "tp"),
        P(None, "dp", "tp"),
        P(None, "dp", "tp"),
        P(None, "dp", "tp"),
        P(None, "dp", None),
        P(None, "tp"),
        P(None, "tp"),
        P(None, "tp"),
        P(None, None, None, "tp"),
        P(None, "tp"),
        P(None, "tp", "dp"),
        P(None, "dp", "tp", None),
        P(None, "dp", None, None, "tp"),
    )
    out_specs = (P(None, "dp"), P(None, "dp", "tp", None), P(None, "dp", None, None, "tp"))
    body = functools.partial(per_device, mesh.shape["dp"], mesh.shape["tp"])
    return jax.shard_map(
        body, mesh=mesh, in_specs=in_specs, out_specs=out_specs, check_vma=False
    )
```
